32 devices in a mesh: sp: 8 (over z, x), tp: 4 (over y, core).
Axes of the slice: x: 2, y: 2, z: 4, core: 2. Of those that a mesh axis runs over, the one named last changes fastest.
Arguments:
- residual: bfloat16 [2048, 2048], P(('sp', 'tp')), may hold values from -6 to 6
- queries: bfloat16 [2048, 1024], P('sp', 'tp'), may hold values from -8 to 8
- key_pairs: bfloat16 [2048, 512], P('sp', 'tp'), may hold values from -8 to 8
- values: bfloat16 [2048, 512], P('sp', 'tp'), may hold values from -6 to 6
- lambdas: float32 [8], P('tp'), may hold values from 0.3 to 0.8
- head_gain: float32 [128], replicated, may hold values from 0.1 to 1.9
- out_weight: bfloat16 [1024, 2048], replicated, may hold values from -0.1875 to 0.1875
- mixer_gain: float32 [2048], replicated, may hold values from 0.1 to 1.9
- before_gain: float32 [2048], replicated, may hold values from 0.1 to 1.9
- after_gain: float32 [2048], replicated, may hold values from 0.1 to 1.9
- gate_weight: bfloat16 [2048, 5632], P('sp', 'tp'), may hold values from -0.125 to 0.125
- up_weight: bfloat16 [2048, 5632], P('sp', 'tp'), may hold values from -0.125 to 0.125
- down_weight: bfloat16 [5632, 2048], P('tp', 'sp'), may hold values from -0.078125 to 0.078125
Outputs:
- updated: bfloat16 [2048, 2048], P(('sp', 'tp'))
The draws below stay inside these ranges and needn't reach their ends.
All inputs are finite; a program needn't handle non-finite values.
Results may differ from the reference program's by a relative error of at most 0.014.
Values may be sent and summed in bfloat16 or wider, within the bound.
A program may use at most 128 MiB of HBM per device.

```python
import math
import jax
import jax.numpy as jnp
from jax import lax

D = 2048
FF = 5632
HEADS = 8
KV_HEADS = 4
HEAD_DIM = 64
TOKENS = 2048
N_TP = 4


def drawn_pair(key):
    query_key, key_key = jax.random.split(key, 2)
    query_draw = jnp.clip(1.3 * jax.random.normal(query_key, (TOKENS, HEADS, 2, HEAD_DIM), jnp.float32), -7.5, 7.5)
    key_draw = jnp.clip(1.3 * jax.random.normal(key_key, (TOKENS, KV_HEADS, 2, HEAD_DIM), jnp.float32), -7.5, 7.5)
    return (query_draw, key_draw)


def draw_queries(key, part):
    query_draw = drawn_pair(jax.random.fold_in(key, 17))[0]
    return query_draw.reshape(TOKENS, HEADS * 2 * HEAD_DIM).astype(jnp.bfloat16)


def draw_key_pairs(key, part):
    key_draw = drawn_pair(jax.random.fold_in(key, 17))[1]
    return key_draw.reshape(TOKENS, KV_HEADS * 2 * HEAD_DIM).astype(jnp.bfloat16)


def level_of(rng, dims, cuts, low, largest):
    loudness, own = 1.0, jax.random.fold_in(rng, 6)
    for axis_at, shards_of in cuts:
        draws = jnp.exp(jax.random.uniform(jax.random.fold_in(own, axis_at), (shards_of,), jnp.float32, low / len(cuts), largest / len(cuts)))
        loudness = loudness * jnp.repeat(draws, dims[axis_at] // shards_of).reshape([-1 if axis == axis_at else 1 for axis in range(len(dims))])
    return loudness


def normal_values(own_key, shape, scale, bound, shards=(), held_as=jnp.bfloat16):
    level = level_of(own_key, shape, shards, -0.22, 0.18) if shards else 1.0
    values = jax.random.normal(own_key, shape, jnp.float32) * scale * level
    return jnp.minimum(jnp.maximum(values, -bound), bound).astype(held_as)


def setup_inputs(seed: int = 0) -> dict:
    arg_keys = jax.random.split(jax.random.key(seed), 14)
    residual = normal_values(arg_keys[0], (TOKENS, D), 1.0, 6.0, ((0, 32),))
    queries = draw_queries(jax.random.fold_in(arg_keys[13], 71), 0)
    key_pairs = draw_key_pairs(jax.random.fold_in(arg_keys[13], 71), 0)
    values = normal_values(arg_keys[3], (TOKENS, KV_HEADS * 2 * HEAD_DIM), 1.0, 6.0, ((0, 8), (1, 4)))
    lambdas = jnp.clip(0.3 + 0.5 * jax.random.uniform(arg_keys[4], (HEADS,), jnp.float32) ** level_of(arg_keys[4], (HEADS,), ((0, 4),), -0.2, 0.2), 0.3, 0.8)
    head_gain = jnp.clip(1.0 + 0.18 * jax.random.normal(arg_keys[5], (2 * HEAD_DIM,), jnp.float32), 0.1, 1.9)
    out_weight = normal_values(arg_keys[6], (HEADS * 2 * HEAD_DIM, D), (HEADS * 2 * HEAD_DIM) ** -0.5, 0.1875)
    mixer_gain = jnp.clip(1.0 + 0.18 * jax.random.normal(arg_keys[7], (D,), jnp.float32), 0.1, 1.9)
    before_gain = jnp.clip(1.0 + 0.18 * jax.random.normal(arg_keys[8], (D,), jnp.float32), 0.1, 1.9)
    after_gain = jnp.clip(1.0 + 0.18 * jax.random.normal(arg_keys[9], (D,), jnp.float32), 0.1, 1.9)
    gate_weight = normal_values(arg_keys[10], (D, FF), D ** -0.5, 0.125, ((0, 8), (1, 4)))
    up_weight = normal_values(arg_keys[11], (D, FF), D ** -0.5, 0.125, ((0, 8), (1, 4)))
    down_weight = normal_values(arg_keys[12], (FF, D), FF ** -0.5, 0.078125, ((0, 4), (1, 8)))
    return {"residual": residual, "queries": queries, "key_pairs": key_pairs, "values": values, "lambdas": lambdas, "head_gain": head_gain, "out_weight": out_weight, "mixer_gain": mixer_gain, "before_gain": before_gain, "after_gain": after_gain, "gate_weight": gate_weight, "up_weight": up_weight, "down_weight": down_weight}


def row_norm(values_in, gain, epsilon):
    mean_square = lax.optimization_barrier(jnp.mean(values_in * values_in, axis=-1, keepdims=True))
    return values_in * lax.rsqrt(mean_square + epsilon) * gain

def reference(residual, queries, key_pairs, values, lambdas, head_gain, out_weight, mixer_gain, before_gain, after_gain, gate_weight, up_weight, down_weight):
    group = HEADS // KV_HEADS
    scale = 1.0 / math.sqrt(HEAD_DIM)
    width = 2 * HEAD_DIM
    query_heads = jnp.transpose(queries.reshape(TOKENS, HEADS, 2, HEAD_DIM), (1, 2, 0, 3))
    key_heads = jnp.transpose(key_pairs.reshape(TOKENS, KV_HEADS, 2, HEAD_DIM), (1, 2, 0, 3))
    value_heads = jnp.transpose(values.reshape(TOKENS, KV_HEADS, width), (1, 0, 2))
    height = math.gcd(TOKENS, 512)
    blocks = TOKENS // height

    def one_block(index):
        head = index // blocks
        first = index % blocks * height
        shared = head // group
        zero = jnp.zeros((), jnp.int32)
        query_block = lax.dynamic_slice(query_heads, (head, zero, first, zero), (1, 2, height, HEAD_DIM))[0]
        key_block = lax.dynamic_index_in_dim(key_heads, shared, 0, keepdims=False)
        value_block = lax.dynamic_index_in_dim(value_heads, shared, 0, keepdims=False)
        second_weight = lax.dynamic_index_in_dim(lambdas, head, 0, keepdims=False)
        results = []
        for which in range(2):
            score = jnp.dot(query_block[which], key_block[which].T, preferred_element_type=jnp.float32) * scale
            top = lax.optimization_barrier(jnp.max(score, axis=1, keepdims=True))
            expo = jnp.exp(score - top)
            total = lax.optimization_barrier(jnp.sum(expo, axis=1, keepdims=True))
            numer = jnp.dot(expo.astype(jnp.bfloat16), value_block, preferred_element_type=jnp.float32)
            results.append(numer / total)
        attended = results[0] - second_weight * results[1]
        return row_norm(attended, head_gain, 1e-05).astype(jnp.bfloat16)
    normed = lax.map(one_block, jnp.arange(HEADS * blocks, dtype=jnp.int32))
    head_out = jnp.transpose(normed.reshape(HEADS, TOKENS, width), (1, 0, 2)).reshape(TOKENS, HEADS * width)
    mixed = jnp.dot(head_out, out_weight, preferred_element_type=jnp.float32).astype(jnp.bfloat16)
    stream = residual.astype(jnp.float32) + row_norm(mixed.astype(jnp.float32), mixer_gain, 1e-06)
    normed_in = row_norm(stream, before_gain, 1e-06).astype(jnp.bfloat16)
    gate = jnp.dot(normed_in, gate_weight, preferred_element_type=jnp.float32)
    up = jnp.dot(normed_in, up_weight, preferred_element_type=jnp.float32)
    hidden = (jax.nn.silu(gate) * up).astype(jnp.bfloat16)
    group_width = FF // N_TP
    channel = jnp.zeros((TOKENS, D), jnp.float32)
    for member in range(N_TP):
        lower = member * group_width
        upper = lower + group_width
        term = jnp.dot(hidden[:, lower:upper], down_weight[lower:upper], preferred_element_type=jnp.float32).astype(jnp.bfloat16)
        channel = channel + lax.optimization_barrier(term).astype(jnp.float32)
    channel = channel.astype(jnp.bfloat16)
    updated = stream + 0.5 * row_norm(channel.astype(jnp.float32), after_gain, 1e-06)
    return updated.astype(jnp.bfloat16)
```

```python
import math

import jax
import jax.numpy as jnp
from jax import lax
from jax.experimental import pallas as pl
from jax.experimental.pallas import tpu as pltpu
from jax.sharding import PartitionSpec as P

HEAD_DIM = 64


def row_norm(values_in, gain, epsilon):
    mean_square = jnp.mean(values_in * values_in, axis=-1, keepdims=True)
    return values_in * lax.rsqrt(mean_square + epsilon) * gain


def on_device(
    residual,
    queries,
    key_pairs,
    values,
    lambdas,
    head_gain,
    out_weight,
    mixer_gain,
    before_gain,
    after_gain,
    gate_weight,
    up_weight,
    down_weight,
):
    tokens_here = queries.shape[0]
    quarter = residual.shape[0]
    width = 2 * HEAD_DIM
    local_heads = queries.shape[1] // width
    scale = 1.0 / math.sqrt(HEAD_DIM)
    height = local_heads * tokens_here
    query_rows = jnp.transpose(
        queries.reshape(tokens_here, local_heads, 2, HEAD_DIM), (2, 1, 0, 3)
    ).reshape(2, height, HEAD_DIM)
    empty = (
        jnp.full((height,), -1e30, jnp.float32),
        jnp.zeros((height,), jnp.float32),
        jnp.zeros((height, width), jnp.float32),
    )
    state = (empty, empty)
    key_piece = lax.all_gather(key_pairs, "sp", axis=0, tiled=True)
    value_piece = lax.all_gather(values, "sp", axis=0, tiled=True)
    length = key_piece.shape[0]
    span = length
    for split_count in range(1, length + 1):
        if length % split_count == 0 and length // split_count <= 2048:
            span = length // split_count
            break
    key_blocks = key_piece.reshape(length // span, span, 2, HEAD_DIM)
    value_blocks = value_piece.reshape(length // span, span, width)

    def advance(carry, blocks_in):
        key_block, value_block = blocks_in
        renewed = []
        for which in range(2):
            running_top, running_total, running_numer = carry[which]
            score = (
                jnp.dot(
                    query_rows[which], key_block[:, which].T, preferred_element_type=jnp.float32
                )
                * scale
            )
            new_top = jnp.maximum(running_top, jnp.max(score, axis=1))
            shrink = jnp.exp(running_top - new_top)
            expo = jnp.exp(score - new_top[:, None])
            new_total = running_total * shrink + jnp.sum(expo, axis=1)
            new_numer = running_numer * shrink[:, None] + jnp.dot(
                expo.astype(jnp.bfloat16), value_block, preferred_element_type=jnp.float32
            )
            renewed.append((new_top, new_total, new_numer))
        return (tuple(renewed), None)

    state, _ = lax.scan(advance, state, (key_blocks, value_blocks))
    first_map, second_map = state
    lambda_rows = jnp.repeat(lambdas, tokens_here)[:, None]
    attended = first_map[2] / first_map[1][:, None] - lambda_rows * (
        second_map[2] / second_map[1][:, None]
    )
    normed = row_norm(attended, head_gain, 1e-05).astype(jnp.bfloat16)
    head_out = jnp.transpose(normed.reshape(local_heads, tokens_here, width), (1, 0, 2)).reshape(
        tokens_here, local_heads * width
    )
    grouped = head_out.reshape(lax.axis_size("tp"), quarter, local_heads * width)
    mixed = jnp.dot(
        lax.all_to_all(grouped, "tp", split_axis=0, concat_axis=2, tiled=True)[0],
        out_weight,
        preferred_element_type=jnp.float32,
    ).astype(jnp.bfloat16)[None][0]
    stream = residual.astype(jnp.float32) + row_norm(mixed.astype(jnp.float32), mixer_gain, 1e-06)
    normed_in = row_norm(stream, before_gain, 1e-06).astype(jnp.bfloat16)
    gathered = lax.all_gather(normed_in, "tp", axis=0, tiled=True)
    empty_hidden = jnp.zeros((gathered.shape[0], gate_weight.shape[1]), jnp.float32)
    pieces = (
        lax.all_gather(gate_weight, "sp", axis=0, tiled=True),
        lax.all_gather(up_weight, "sp", axis=0, tiled=True),
    )
    columns = lax.slice_in_dim(gathered, 0, pieces[0].shape[0], axis=1)
    gate_part = jnp.dot(columns, pieces[0], preferred_element_type=jnp.float32)
    up_part = jnp.dot(columns, pieces[1], preferred_element_type=jnp.float32)
    gate = empty_hidden + gate_part
    up = empty_hidden + up_part
    down_whole = lax.all_gather(down_weight, "sp", axis=1, tiled=True)
    hidden = (jax.nn.silu(gate) * up).astype(jnp.bfloat16)
    picked = lax.slice_in_dim(hidden, 0, lax.axis_size("tp") * quarter, axis=0)
    channel = lax.psum_scatter(
        jnp.dot(picked, down_whole, preferred_element_type=jnp.float32).astype(jnp.bfloat16),
        "tp",
        scatter_dimension=0,
        tiled=True,
    )
    updated = stream + 0.5 * row_norm(channel.astype(jnp.float32), after_gain, 1e-06)
    return updated.astype(jnp.bfloat16)


MESH = pl.DeviceIdType.MESH


def flip(index, bits):
    bit = 1
    while bit <= bits:
        if bits & bit:
            index = index + bit - 2 * bit * ((index // bit) % 2)
        bit *= 2
    return index


PIECES = 2


def layer(
    residual_in,
    queries_in,
    key_in,
    value_in,
    lambdas,
    head_gain,
    out_in,
    mixer_gain,
    before_gain,
    after_gain,
    gate_all,
    up_all,
    down_in,
    updated,
    residual,
    queries,
    out_weight,
    gate_raw,
    up_raw,
    gate_in,
    up_in,
    hidden,
    gate_sum,
    up_sum,
    kv,
    rows_q,
    tops,
    numers,
    gate_w,
    up_w,
    down_w,
    head_out,
    head_in,
    mixed,
    stream,
    x,
    p,
    from_core,
    from_y,
    from_low,
    from_high,
    send_sems,
    recv_sems,
    local_sems,
):
    depth = down_in.shape[0]
    n_tp = head_in.shape[0]
    quarter, width_all = residual.shape
    width = 2 * HEAD_DIM
    heads = queries.shape[1] // width
    tokens_here = queries.shape[0]
    place, member = lax.axis_index("sp"), lax.axis_index("tp")
    used = [0]
    copies = []

    def send(src, dst, axis, bits):
        at = used[0]
        used[0] += 1
        target = flip(place if axis == "sp" else member, bits)
        copy = pltpu.make_async_remote_copy(
            src_ref=src,
            dst_ref=dst,
            send_sem=send_sems.at[at],
            recv_sem=recv_sems.at[at],
            device_id={axis: target},
            device_id_type=MESH,
        )
        copy.start()
        copies.append(copy)
        return copy

    partners = [("sp", 1)] + [("sp", 2 * j) for j in range(1, depth)]
    partners += [("tp", j) for j in range(1, n_tp)]
    barrier = pltpu.get_barrier_semaphore()
    for axis, bits in partners:
        target = flip(place if axis == "sp" else member, bits)
        pl.semaphore_signal(barrier, inc=1, device_id={axis: target}, device_id_type=MESH)

    fetches = []
    for src, dst in (
        (key_in, kv.at[0, :, pl.ds(0, width)]),
        (value_in, kv.at[0, :, pl.ds(width, width)]),
        (queries_in, queries),
        (gate_all, gate_raw),
        (up_all, up_raw),
        (residual_in, residual),
        (out_in, out_weight),
    ):
        fetch = pltpu.make_async_copy(src, dst, local_sems.at[3 + len(fetches)])
        fetch.start()
        fetches.append(fetch)
    fetches[0].wait()
    fetches[1].wait()
    pl.semaphore_wait(barrier, len(partners))

    near = send(kv.at[0], kv.at[1], "sp", 2)
    far = send(kv.at[0], kv.at[2], "sp", 4)
    kv_x = [send(kv.at[0], kv.at[depth], "sp", 1)]

    fetches[2].wait()
    lane = lax.broadcasted_iota(jnp.int32, (tokens_here, width), 1)
    for h in range(heads):
        both = queries[:, h * width : (h + 1) * width].astype(jnp.float32) * (
            1.0 / math.sqrt(HEAD_DIM)
        )
        for which in range(2):
            inside = (lane < HEAD_DIM) if which == 0 else (lane >= HEAD_DIM)
            rows_q[2 * h + which] = jnp.where(inside, both, 0.0).astype(jnp.bfloat16)
    for source, target, fetch in ((gate_raw, gate_in, fetches[3]), (up_raw, up_in, fetches[4])):
        fetch.wait()
        columns = target.shape[2]
        for j in range(depth):
            target[j] = source[:, j * columns : (j + 1) * columns]

    def attend(slots, first):
        keys = jnp.concatenate([kv[slot, :, :width] for slot in slots], axis=0)
        vals = jnp.concatenate([kv[slot, :, width:] for slot in slots], axis=0)
        vals = jnp.concatenate([vals, jnp.ones_like(vals)], axis=1)

        def unit(u, _):
            score = lax.dot_general(
                rows_q[u], keys, (((1,), (1,)), ((), ())), preferred_element_type=jnp.float32
            )
            top = jnp.max(score, axis=1, keepdims=True)
            if not first:
                old = tops[u][:, :1]
                top = jnp.maximum(old, top)
            expo = jnp.exp(score - top).astype(jnp.bfloat16)
            numer = jnp.dot(expo, vals, preferred_element_type=jnp.float32)
            if not first:
                numer = numers[u] * jnp.exp(old - top) + numer
            numers[u] = numer
            tops[u] = jnp.broadcast_to(top, tops.shape[1:])
            return 0

        for u in range(2 * heads):
            unit(u, 0)

    kv_x[0].wait_recv()
    attend((0, depth), True)
    lane_x, low = place % 2, place // 2
    upper = low // 2
    inner = (upper + low % 2) % 2
    mirror = 1 - inner
    pairs = [(j, flip(place, 2 * j) // 2) for j in range(1, depth)]
    crossing = [(2 + inner, 2 - upper), (2 + mirror, 3 - 3 * upper)]

    def plan_z(source, target):
        base = used[0]
        used[0] += (depth - 1) * PIECES
        rows = target.shape[1] // PIECES

        def move(j, goal, k):
            at = base + (j - 1) * PIECES + k
            part = pl.ds(k * rows, rows)
            return pltpu.make_async_remote_copy(
                src_ref=source.at[goal, part],
                dst_ref=target.at[place, part],
                send_sem=send_sems.at[at],
                recv_sem=recv_sems.at[at],
                device_id={"sp": 2 * goal + lane_x},
                device_id_type=MESH,
            )

        def begin(order):
            for j, goal in order:
                for k in range(PIECES):
                    move(j, goal, k).start()

        moves = {(j, k): move(j, goal, k) for j, goal in pairs for k in range(PIECES)}
        copies.extend(moves.values())
        return moves, begin

    def scatter_x(source, target, at):
        mine = source.at[place // 2]
        local = pltpu.make_async_copy(mine, target.at[place], local_sems.at[at])
        local.start()
        return local, send(mine, target.at[place], "sp", 1)

    def forward(target, over_z, j):
        rows = target.shape[1] // PIECES
        over_x = []
        for k in range(PIECES):
            over_z[j, k].wait_recv()
            slot = target.at[flip(place, 2 * j), pl.ds(k * rows, rows)]
            over_x.append(send(slot, slot, "sp", 1))
        return over_x

    def arrived(group):
        for copy in group:
            copy.wait_recv()

    near.wait_recv()
    kv_x.append(send(kv.at[1], kv.at[depth + 1], "sp", 1))
    far.wait_recv()
    relayed = send(kv.at[2], kv.at[3], "sp", 2)
    kv_x.append(send(kv.at[2], kv.at[depth + 2], "sp", 1))
    gate_z, begin_gate = plan_z(gate_in, gate_w)
    begin_gate(crossing[:1])
    kv_x[1].wait_recv()
    attend((1, depth + 1), False)
    relayed.wait_recv()
    kv_x.append(send(kv.at[3], kv.at[depth + 3], "sp", 1))
    begin_gate(crossing[1:] + pairs[:1])
    gate_own = scatter_x(gate_in, gate_w, 0)
    kv_x[2].wait_recv()
    attend((2, depth + 2), False)
    kv_x[3].wait_recv()
    attend((3, depth + 3), False)

    for h in range(heads):
        parts = []
        for which in range(2):
            whole = numers[2 * h + which]
            parts.append(whole[:, :width] / whole[:, width:])
        attended = parts[0] - lambdas[h] * parts[1]
        normed = row_norm(attended, head_gain[...], 1e-05).astype(jnp.bfloat16)
        for t in range(n_tp):
            head_out[t, :, h * width : (h + 1) * width] = normed[t * quarter : (t + 1) * quarter]
    moved = [send(head_out.at[flip(member, j)], head_in.at[member], "tp", j) for j in range(1, n_tp)]
    head_in[member] = head_out[member]
    fetches[5].wait()
    fetches[6].wait()
    step = head_in.shape[2]

    def project(m):
        rows = pl.ds(pl.multiple_of(m * step, step), step)
        return jnp.dot(head_in[m], out_weight[rows], preferred_element_type=jnp.float32)

    mixed[...] = project(member)
    for j, copy in zip(range(1, n_tp), moved):
        copy.wait_recv()
        mixed[...] += project(flip(member, j))
    rounded = mixed[...].astype(jnp.bfloat16).astype(jnp.float32)
    stream[...] = residual[...].astype(jnp.float32) + row_norm(rounded, mixer_gain[...], 1e-06)
    x[0] = row_norm(stream[...], before_gain[...], 1e-06).astype(jnp.bfloat16)

    half = 2 * depth
    bands = [pl.ds(k * (quarter // PIECES), quarter // PIECES) for k in range(PIECES)]

    def send_tile(origin, goal, axis, bits):
        return [send(x.at[origin, band], x.at[goal, band], axis, bits) for band in bands]

    def relay_tile(arriving, origin, *routes):
        moves = [[] for _ in routes]
        for copy, band in zip(arriving, bands):
            copy.wait_recv()
            for route, made in zip(routes, moves):
                goal, axis, bits = route
                made.append(send(x.at[origin, band], x.at[goal, band], axis, bits))
        return moves

    near = send_tile(0, 1, "sp", 2)
    far = send_tile(0, 2, "sp", 4)
    x_c = [send_tile(0, half, "tp", 1)]
    x_y = [send_tile(0, depth, "tp", 2)]
    gate_x = [forward(gate_w, gate_z, j) for j in (1, 2, 3)]
    up_own = scatter_x(up_in, up_w, 1)
    for made, group in zip(
        relay_tile(near, 1, (depth + 1, "tp", 2), (half + 1, "tp", 1)), (x_y, x_c)
    ):
        group.append(made)
    relayed, made_y, made_c = relay_tile(
        far, 2, (3, "sp", 2), (depth + 2, "tp", 2), (half + 2, "tp", 1)
    )
    x_y.append(made_y)
    x_c.append(made_c)
    up_z, begin_up = plan_z(up_in, up_w)
    begin_up(crossing[:1])
    for made, group in zip(
        relay_tile(relayed, 3, (depth + 3, "tp", 2), (half + 3, "tp", 1)), (x_y, x_c)
    ):
        group.append(made)
    begin_up(pairs[:1] + crossing[1:])
    down_z, begin_down = plan_z(down_in, down_w)
    begin_down(crossing[:1])
    down_own = scatter_x(down_in, down_w, 2)

    units = gate_w.shape[2]
    span = down_w.shape[2]
    inner_rows = gate_w.shape[1]
    rows_group = depth * quarter

    def source_of(j):
        return low if j == 0 else flip(place, 2 * j) // 2

    def multiply(w, total, j, g, first):
        begin = 2 * source_of(j)
        columns = pl.ds(pl.multiple_of(begin * inner_rows, 2 * inner_rows), 2 * inner_rows)
        rows = x[g * depth : (g + 1) * depth, :, columns].reshape(rows_group, 2 * inner_rows)
        weights = w[pl.ds(begin, 2)].reshape(2 * inner_rows, units)
        part = jnp.dot(rows, weights, preferred_element_type=jnp.float32)
        total[g] = part if first else total[g] + part

    def multiply_all(w, total, g, sources):
        for j in sources:
            multiply(w, total, j, g, j == 0)

    def finish_hidden(g):
        gate, up = gate_sum[g], up_sum[g]
        hidden[g] = (gate / (1.0 + jnp.exp(-gate)) * up).astype(jnp.bfloat16)

    gate_own[0].wait()
    gate_own[1].wait_recv()
    for group in gate_x:
        arrived(group)
    multiply_all(gate_w, gate_sum, 0, range(depth))
    x_last = []

    def pass_on(j):
        x_last.extend(relay_tile(x_y[j], depth + j, (half + depth + j, "tp", 1)))

    pass_on(0)
    pass_on(1)
    up_x = [forward(up_w, up_z, 1)]
    for group in x_c:
        arrived(group)
    multiply_all(gate_w, gate_sum, 2, range(depth))
    pass_on(2)
    up_x.append(forward(up_w, up_z, 2))
    pass_on(3)
    up_x.append(forward(up_w, up_z, 3))
    begin_down(pairs[:1] + crossing[1:])
    multiply_all(gate_w, gate_sum, 1, range(depth))
    up_own[0].wait()
    up_own[1].wait_recv()
    for g in (0, 1, 2):
        multiply_all(up_w, up_sum, g, (0,))
    for group in x_last:
        arrived(group)
    multiply_all(gate_w, gate_sum, 3, range(depth))
    multiply_all(up_w, up_sum, 3, (0,))
    arrived(up_x[0])
    for g in range(4):
        multiply_all(up_w, up_sum, g, (1,))
    arrived(up_x[1])
    for g in range(4):
        multiply_all(up_w, up_sum, g, (2,))
    arrived(up_x[2])
    for g in range(4):
        multiply_all(up_w, up_sum, g, (3,))
        finish_hidden(g)
    down_own[0].wait()

    def block_of(j, m):
        return 2 * source_of(j) + (lane_x if m == 0 else 1 - lane_x)

    def narrow(j, m, g):
        part = jnp.dot(hidden[g], down_w[block_of(j, m)], preferred_element_type=jnp.float32)
        p[j, m, g * depth : (g + 1) * depth] = part.astype(jnp.bfloat16).reshape(
            depth, quarter, span
        )

    core_y, core_own, over_y, over_low, over_high = {}, {}, {}, {}, {}

    def narrow_all(j, m):
        at = j, m
        narrow(j, m, 3)
        core_y[at] = send(
            p.at[j, m, pl.ds(3 * depth, depth)], from_core.at[j, m, pl.ds(depth, depth)], "tp", 1
        )
        narrow(j, m, 1)
        narrow(j, m, 2)
        core_own[at] = send(
            p.at[j, m, pl.ds(2 * depth, depth)], from_core.at[j, m, pl.ds(0, depth)], "tp", 1
        )
        narrow(j, m, 0)

    def send_y(j, m):
        at = j, m
        core_y[at].wait_recv()
        p[j, m, depth : 2 * depth] = (
            p[j, m, depth : 2 * depth].astype(jnp.float32)
            + from_core[j, m, depth : 2 * depth].astype(jnp.float32)
        ).astype(jnp.bfloat16)
        over_y[at] = send(p.at[j, m, pl.ds(depth, depth)], from_y.at[j, m], "tp", 2)

    def sum_y(j, m):
        at = j, m
        core_own[at].wait_recv()
        over_y[at].wait_recv()
        p[j, m, :depth] = (
            p[j, m, :depth].astype(jnp.float32)
            + from_core[j, m, :depth].astype(jnp.float32)
            + from_y[j, m].astype(jnp.float32)
        ).astype(jnp.bfloat16)
        over_low[at] = [
            send(p.at[j, m, t], from_low.at[j ^ 1, m, t // 2], "sp", 2) for t in (3, 1)
        ]

    def sum_low(j, m):
        for copy in over_low[j ^ 1, m]:
            copy.wait_recv()
        p[j, m, 2] = (
            p[j, m, 2].astype(jnp.float32) + from_low[j, m, 1].astype(jnp.float32)
        ).astype(jnp.bfloat16)
        over_high[j, m] = send(p.at[j, m, 2], from_high.at[j ^ 2, m], "sp", 4)

    def sum_high(j, m):
        over_high[j ^ 2, m].wait_recv()
        columns = pl.ds(pl.multiple_of(block_of(j, m) * span, span), span)
        mixed[:, columns] = (
            p[j, m, 0].astype(jnp.float32)
            + from_low[j, m, 0].astype(jnp.float32)
            + from_high[j, m].astype(jnp.float32)
        )

    down_x = [forward(down_w, down_z, 1)]
    narrow_all(0, 0)
    down_own[1].wait_recv()
    narrow_all(0, 1)
    send_y(0, 0)
    narrow_all(1, 0)
    send_y(0, 1)
    arrived(down_x[0])
    narrow_all(1, 1)
    send_y(1, 0)
    down_x.append(forward(down_w, down_z, 2))
    send_y(1, 1)
    narrow_all(2, 0)
    sum_y(0, 0)
    down_x.append(forward(down_w, down_z, 3))
    send_y(2, 0)
    narrow_all(3, 0)
    sum_y(0, 1)
    arrived(down_x[1])
    narrow_all(2, 1)
    send_y(3, 0)
    arrived(down_x[2])
    narrow_all(3, 1)
    send_y(2, 1)
    sum_y(1, 0)
    send_y(3, 1)
    sum_y(1, 1)
    sum_y(2, 0)
    sum_low(0, 0)
    sum_low(1, 0)
    sum_y(3, 0)
    sum_low(0, 1)
    sum_low(1, 1)
    sum_y(2, 1)
    sum_y(3, 1)
    sum_low(2, 0)
    sum_low(3, 0)
    sum_low(2, 1)
    sum_low(3, 1)
    for j in range(depth):
        sum_high(j, 0)
    for j in range(depth):
        sum_high(j, 1)
    channel = mixed[...].astype(jnp.bfloat16).astype(jnp.float32)
    updated[...] = (stream[...] + 0.5 * row_norm(channel, after_gain[...], 1e-06)).astype(
        updated.dtype
    )
    for copy in copies:
        copy.wait_send()


def one_kernel(
    residual,
    queries,
    key_pairs,
    values,
    lambdas,
    head_gain,
    out_weight,
    mixer_gain,
    before_gain,
    after_gain,
    gate_weight,
    up_weight,
    down_weight,
):
    n_sp, n_tp = lax.axis_size("sp"), lax.axis_size("tp")
    depth = n_sp // 2
    quarter, width_all = residual.shape
    tokens_here, query_width = queries.shape
    width = 2 * HEAD_DIM
    maps = query_width // HEAD_DIM
    inner, units_all = gate_weight.shape
    units = units_all // depth
    span = down_weight.shape[1]
    down_in = down_weight.reshape(depth, units, span)
    tiles = 4 * depth
    weight_sends = 3 * (1 + 2 * (depth - 1) * PIECES)
    tile_sends = (depth - 1 + 3 * depth) * PIECES
    total_sends = 2 * depth - 1 + tile_sends + weight_sends + n_tp - 1 + 12 * depth
    vmem = pl.BlockSpec(memory_space=pltpu.VMEM)
    hbm = pl.BlockSpec(memory_space=pl.ANY)
    smem = pl.BlockSpec(memory_space=pltpu.SMEM)
    bf16 = jnp.bfloat16
    f32 = jnp.float32
    return pl.pallas_call(
        layer,
        out_shape=jax.ShapeDtypeStruct(residual.shape, bf16),
        in_specs=[hbm] * 4 + [smem, vmem, hbm] + [vmem] * 3 + [hbm] * 3,
        out_specs=vmem,
        scratch_shapes=[
            pltpu.VMEM(residual.shape, bf16),
            pltpu.VMEM(queries.shape, bf16),
            pltpu.VMEM(out_weight.shape, bf16),
            pltpu.VMEM(gate_weight.shape, bf16),
            pltpu.VMEM(up_weight.shape, bf16),
            pltpu.VMEM((depth, inner, units), bf16),
            pltpu.VMEM((depth, inner, units), bf16),
            pltpu.VMEM((4, depth * quarter, units), bf16),
            pltpu.VMEM((4, depth * quarter, units), f32),
            pltpu.VMEM((4, depth * quarter, units), f32),
            pltpu.VMEM((n_sp, tokens_here, 2 * key_pairs.shape[1]), bf16),
            pltpu.VMEM((maps, tokens_here, width), bf16),
            pltpu.VMEM((maps, tokens_here, width), f32),
            pltpu.VMEM((maps, tokens_here, 2 * width), f32),
            pltpu.VMEM((n_sp, inner, units), bf16),
            pltpu.VMEM((n_sp, inner, units), bf16),
            pltpu.VMEM((n_sp, units, span), bf16),
            pltpu.VMEM((n_tp, quarter, query_width), bf16),
            pltpu.VMEM((n_tp, quarter, query_width), bf16),
            pltpu.VMEM((quarter, width_all), f32),
            pltpu.VMEM((quarter, width_all), f32),
            pltpu.VMEM((tiles, quarter, width_all), bf16),
            pltpu.VMEM((depth, 2, tiles, quarter, span), bf16),
            pltpu.VMEM((depth, 2, 2 * depth, quarter, span), bf16),
            pltpu.VMEM((depth, 2, depth, quarter, span), bf16),
            pltpu.VMEM((depth, 2, 2, quarter, span), bf16),
            pltpu.VMEM((depth, 2, quarter, span), bf16),
            pltpu.SemaphoreType.DMA((total_sends,)),
            pltpu.SemaphoreType.DMA((total_sends,)),
            pltpu.SemaphoreType.DMA((10,)),
        ],
        compiler_params=pltpu.CompilerParams(
            collective_id=0, has_side_effects=True, vmem_limit_bytes=60 * 1024 * 1024
        ),
    )(
        residual,
        queries,
        key_pairs,
        values,
        lambdas,
        head_gain[None],
        out_weight,
        mixer_gain[None],
        before_gain[None],
        after_gain[None],
        gate_weight,
        up_weight,
        down_in,
    )


def fits(mesh):
    return mesh.shape["tp"] == 4 and mesh.shape["sp"] == 8


def solution(mesh):
    return jax.shard_map(
        one_kernel if fits(mesh) else on_device,
        mesh=mesh,
        in_specs=(
            P(("sp", "tp"), None),
            P("sp", "tp"),
            P("sp", "tp"),
            P("sp", "tp"),
            P("tp"),
            P(),
            P(),
            P(),
            P(),
            P(),
            P("sp", "tp"),
            P("sp", "tp"),
            P("tp", "sp"),
        ),
        out_specs=P(("sp", "tp"), None),
        check_vma=False,
    )
```
